32 devices in a mesh: sp: 8 (over z, y), tp: 4 (over x, core).
Axes of the slice: x: 2, y: 2, z: 4, core: 2. Of those that a mesh axis runs over, the one named last changes fastest.
Arguments:
- stream: bfloat16 [4096, 2048], P(('sp', 'tp')), may hold values from -6 to 6
- conv_value: bfloat16 [4096, 512], P('sp', 'tp'), may hold values from -6 to 6
- conv_gate: bfloat16 [4096, 512], P('sp', 'tp'), may hold values from -8 to 8
- doc_ids: int32 [4096], P('sp'), may hold values from 0 to 3, never falling along the last dimension, each value on 1 to 2048 neighbouring positions
- conv_taps: float32 [31, 512], P(None, 'tp'), may hold values from -2.2 to 2.2
- conv_bias: float32 [512], P('tp'), may hold values from -3 to 3
- chan_gain: float32 [512], replicated, may hold values from 0.1 to 1.9
- chan_shift: float32 [512], replicated, may hold values from -3 to 3
- out_weight: bfloat16 [512, 2048], replicated, may hold values from -0.25 to 0.25
- rms_gain: float32 [2048], replicated, may hold values from 0.1 to 1.9
- expert_ids: int32 [4096, 2], P(('sp', 'tp')), may hold values from 0 to 15, all different within a row; in each aligned block of 128 rows (0 to 127, 128 to 255, ...) at most 24 rows name the same one
- group_prob: float32 [4096], P(('sp', 'tp')), may hold values from 0.3 to 1
- route_logits: float32 [4096, 2], P(('sp', 'tp')), may hold values from -6 to 6
- expert_gate: bfloat16 [16, 2048, 1024], P('sp', None, 'tp'), may hold values from -0.125 to 0.125
- expert_up: bfloat16 [16, 2048, 1024], P('sp', None, 'tp'), may hold values from -0.125 to 0.125
- expert_down: bfloat16 [16, 1024, 2048], P('sp', 'tp'), may hold values from -0.1875 to 0.1875
Outputs:
- mixed: bfloat16 [4096, 2048], P(('sp', 'tp'))
The draws below stay inside these ranges and needn't reach their ends.
Inputs may be any that keep to these rules, and one draw needn't show every extreme that they name: `expert_ids`: each row names 2 different experts. In each aligned block of 128 rows (the rows of one device) no expert is named by more than 24 rows, a bound that some block reaches. `doc_ids`: document numbers never fall along the sequence; every document has 1 to 2048 positions, one exactly 2048.
All inputs are finite; a program needn't handle non-finite values.
Results may differ from the reference program's by a relative error of at most 0.012.
Values may be sent and summed in bfloat16 or wider, within the bound.
A program may use at most 64 MiB of HBM per device.

```python
import math
import jax
import jax.numpy as jnp
import numpy as np
from jax import lax

D = 2048
CONV_CH = 512
FF = 1024
WIDTH = 31
TOPK = 2
TOK_DEV = 128
EXPERTS = 16
CAP = 24
TOKENS = 4096
DOCS = 4
DOC_MOST = 2048
N_TP = 4


def draw_conv_taps(key, part):
    first, second, third = jax.random.split(jax.random.fold_in(key, 11), 3)
    base = jnp.clip(jax.random.normal(first, (WIDTH, CONV_CH), jnp.float32), -4.0, 4.0)
    levels = jnp.exp(jax.random.uniform(second, (4,), jnp.float32, -1.2, 1.2))
    column = jnp.repeat(levels, CONV_CH // 4)
    jitter = jax.random.uniform(third, (CONV_CH,), jnp.float32, 0.7, 1.0)
    taps = base * (column * jitter)[None, :] * WIDTH ** (-0.5)
    return jnp.clip(taps, -2.2, 2.2)


def steps_of(rng, dims, shards, low, high):
    loudness, own = 1.0, jax.random.fold_in(rng, 6)
    for position, blocks in shards:
        heights = jnp.exp(jax.random.uniform(jax.random.fold_in(own, position), (blocks,), jnp.float32, low / len(shards), high / len(shards)))
        loudness = loudness * jnp.repeat(heights, dims[position] // blocks).reshape([-1 if axis == position else 1 for axis in range(len(dims))])
    return loudness


def split_up(amount, total, limit, slope):
    loads = [(1 << 20) // math.isqrt(standing ** slope) + 1 for standing in range(2, amount + 1)]
    spare, holding = total - limit - (amount - 1), [1] * (amount - 1)
    while spare > 0:
        free = [i for i in range(amount - 1) if holding[i] < limit]
        pool, budget = sum([loads[i] for i in free]), spare
        for i in free:
            more = min(limit - holding[i], max(1, budget * loads[i] // pool), spare)
            holding[i] = holding[i] + more
            spare = spare - more
    return np.array([limit] + holding)


def ragged_sizes(own_key, number_of, total, most, lean):
    if number_of == 2:
        one = jax.random.randint(own_key, (), max(1, total - most), min(most, total - 1) + 1)
        return jnp.stack([one, total - one])
    tallies = jnp.asarray(split_up(number_of, total, most, lean), jnp.int32)
    pairs = (number_of - 1) // 2
    source_of, taker = tallies[1:1 + 2 * pairs:2], tallies[2:2 + 2 * pairs:2]
    margin = jnp.minimum(source_of - 1, most - taker)
    passed = jax.random.randint(jax.random.fold_in(own_key, 1), (pairs,), 0, 1 << 20) % (margin + 1)
    tallies = tallies.at[1:1 + 2 * pairs:2].set(source_of - passed).at[2:2 + 2 * pairs:2].set(taker + passed)
    return tallies[jax.random.permutation(jax.random.fold_in(own_key, 2), number_of)]


def shared_out(own_key, own, number, rows, count, top, limit, lean):
    order = jax.random.permutation(own_key, count)
    heavy_load, ordinary = portions_of(count, rows * top, limit, lean, True), portions_of(count, rows * top, limit, lean, False)
    places = jnp.arange(count)

    def named(tallies, turn):
        used = int((tallies > 0).sum())
        fixed = max(1, used // 4)
        moved = fixed + (places - fixed + turn * (used - fixed)) % max(1, count - fixed)
        return jnp.zeros((count,), jnp.int32).at[order[jnp.where(places < fixed, places, moved)]].set(jnp.asarray(tallies, jnp.int32))

    tallies = jnp.where(number % 4 == 0, named(heavy_load, number // 4), named(ordinary, number - number // 4 - 1))
    mixed = jax.random.permutation(jax.random.fold_in(own, 3), count)
    giver, taker = mixed[0:count // 2 * 2:2], mixed[1:count // 2 * 2:2]
    room = jnp.minimum(tallies[giver] - 1, limit - tallies[taker]) // 2
    room = jnp.where((giver == order[0]) | (taker == order[0]) | (tallies[taker] == 0), 0, jnp.maximum(room, 0))
    moved = jax.random.randint(jax.random.fold_in(own, 4), (count // 2,), 0, 1 << 20) % (room + 1)
    tallies = tallies.at[giver].add(-moved).at[taker].add(moved)
    items = jnp.searchsorted(jnp.cumsum(tallies), jnp.arange(rows * top), side="right").astype(jnp.int32)
    listing = items.reshape(top, rows).T
    listing = listing[jax.random.permutation(jax.random.fold_in(own, 1), rows)]
    turn = jax.random.randint(jax.random.fold_in(own, 2), (rows, 1), 0, top)
    return jnp.take_along_axis(listing, (jnp.arange(top)[None, :] + turn) % top, axis=1)


def portions_of(count, total, most, slope, full):
    portions = [(1 << 20) // math.isqrt(rank ** slope) + 1 for rank in range(1, count + 1)]
    largest = most if full else min(most, max(-(-total // count), total * portions[0] // sum(portions)))
    least = 1 if total - largest >= count - 1 else 0
    given, spare = [largest] + [least] * (count - 1), total - largest - least * (count - 1)
    while spare > 0:
        movable = [i for i in range(1, count) if given[i] < largest] or [i for i in range(1, count) if given[i] < most]
        mass, left = sum([portions[i] for i in movable]), spare
        for i in movable:
            more = min(most - given[i], max(1, left * portions[i] // mass), spare)
            given[i] = given[i] + more
            spare = spare - more
    return np.array(given)


def gaussian(rng, dims, deviation, most, cuts=(), kind=jnp.bfloat16):
    values = deviation * jax.random.normal(rng, dims, jnp.float32)
    if cuts:
        values = values * steps_of(rng, dims, cuts, -0.22, 0.18)
    return jnp.clip(values, -most, most).astype(kind)


def setup_inputs(seed: int = 0) -> dict:
    seeds = jax.random.split(jax.random.key(seed), 17)
    stream = gaussian(seeds[0], (TOKENS, D), 1.0, 6.0, ((0, 32),))
    conv_value = gaussian(seeds[1], (TOKENS, CONV_CH), 1.0, 6.0, ((0, 8), (1, 4)))
    conv_gate = gaussian(seeds[2], (TOKENS, CONV_CH), 1.5, 8.0, ((0, 8), (1, 4)))
    doc_ids = jnp.searchsorted(jnp.cumsum(ragged_sizes(seeds[3], DOCS, TOKENS, DOC_MOST, 0)), jnp.arange(TOKENS), side="right").astype(jnp.int32)
    conv_taps = draw_conv_taps(jax.random.fold_in(seeds[16], 71), 0)
    conv_bias = gaussian(seeds[5], (CONV_CH,), 0.5, 3.0, ((0, 4),), jnp.float32)
    chan_gain = jnp.clip(1.0 + 0.18 * jax.random.normal(seeds[6], (CONV_CH,), jnp.float32), 0.1, 1.9)
    chan_shift = gaussian(seeds[7], (CONV_CH,), 0.5, 3.0, (), jnp.float32)
    out_weight = gaussian(seeds[8], (CONV_CH, D), CONV_CH ** -0.5, 0.25)
    rms_gain = jnp.clip(1.0 + 0.18 * jax.random.normal(seeds[9], (D,), jnp.float32), 0.1, 1.9)
    expert_ids_keys = jax.random.split(jax.random.fold_in(seeds[10], 1), TOKENS // TOK_DEV)
    expert_ids_turns = jax.random.permutation(jax.random.fold_in(seeds[10], 3), TOKENS // TOK_DEV)
    expert_ids = jax.vmap(lambda own, number: shared_out(jax.random.fold_in(seeds[10], 2), own, number, TOK_DEV, EXPERTS, TOPK, CAP, 1))(expert_ids_keys, expert_ids_turns).reshape((TOKENS, TOPK))
    group_prob = jnp.clip(0.3 + 0.7 * jax.random.uniform(seeds[11], (TOKENS,), jnp.float32) ** steps_of(seeds[11], (TOKENS,), ((0, 32),), -0.2, 0.2), 0.3, 1.0)
    route_logits = gaussian(seeds[12], (TOKENS, TOPK), 1.5, 6.0, ((0, 32),), jnp.float32)
    expert_gate = gaussian(seeds[13], (EXPERTS, D, FF), D ** -0.5, 0.125, ((0, 8), (2, 4)))
    expert_up = gaussian(seeds[14], (EXPERTS, D, FF), D ** -0.5, 0.125, ((0, 8), (2, 4)))
    expert_down = gaussian(seeds[15], (EXPERTS, FF, D), FF ** -0.5, 0.1875, ((0, 8), (1, 4)))
    return dict(stream=stream, conv_value=conv_value, conv_gate=conv_gate, doc_ids=doc_ids, conv_taps=conv_taps, conv_bias=conv_bias, chan_gain=chan_gain, chan_shift=chan_shift, out_weight=out_weight, rms_gain=rms_gain, expert_ids=expert_ids, group_prob=group_prob, route_logits=route_logits, expert_gate=expert_gate, expert_up=expert_up, expert_down=expert_down)


eps = 1e-06
row_block = 128

def causal_conv(values, gates, docs, conv_taps, conv_bias):
    reach = conv_taps.shape[0] - 1
    acts = values.astype(jnp.float32) * jax.nn.sigmoid(gates.astype(jnp.float32))
    total = values.shape[0] - reach
    result = jnp.broadcast_to(conv_bias[None, :], (total, values.shape[1])).astype(jnp.float32)
    own_doc = docs[reach:]
    for offset in range(reach + 1):
        begin = reach - offset
        same = (docs[begin:begin + total] == own_doc)[:, None]
        result = result + jnp.where(same, acts[begin:begin + total], 0.0) * conv_taps[offset][None, :]
    return result.astype(jnp.bfloat16)

def channel_norm(conved, chan_gain, chan_shift):
    values = conved.astype(jnp.float32)
    mean = lax.optimization_barrier(jnp.mean(values, axis=-1, keepdims=True))
    square = lax.optimization_barrier(jnp.mean(values * values, axis=-1, keepdims=True))
    spread = square - mean * mean
    scaled = (values - mean) * lax.rsqrt(spread + eps) * chan_gain + chan_shift
    return jax.nn.silu(scaled).astype(jnp.bfloat16)

def rms_norm(resid, rms_gain):
    values = resid.astype(jnp.float32)
    square = lax.optimization_barrier(jnp.mean(values * values, axis=-1, keepdims=True))
    return (values * lax.rsqrt(square + eps) * rms_gain).astype(jnp.bfloat16)

def route_weights(group_prob, route_logits):
    gap = route_logits[:, 0] - route_logits[:, 1]
    return jnp.stack([group_prob * jax.nn.sigmoid(gap), group_prob * jax.nn.sigmoid(-gap)], axis=1)

def run_experts(normed, expert_ids, expert_gate, expert_up, expert_down):
    routes = TOKENS * TOPK
    expert = expert_ids.reshape(routes).astype(jnp.int32)
    token = (jnp.arange(routes, dtype=jnp.int32) // TOPK).astype(jnp.int32)
    order = jnp.argsort(expert, stable=True).astype(jnp.int32)
    sorted_expert = expert[order]
    sorted_token = token[order]
    counts = lax.optimization_barrier(jnp.sum((expert[:, None] == jnp.arange(EXPERTS, dtype=jnp.int32)[None, :]).astype(jnp.int32), axis=0))
    begin = jnp.cumsum(counts) - counts
    padded = (counts + row_block - 1) // row_block * row_block
    pad_end = jnp.cumsum(padded)
    pad_begin = pad_end - padded
    dest = (pad_begin[sorted_expert] + jnp.arange(routes, dtype=jnp.int32) - begin[sorted_expert]).astype(jnp.int32)
    n_rows = (routes + row_block - 1) // row_block * row_block + EXPERTS * row_block
    n_blocks = n_rows // row_block
    row_token = jnp.zeros((n_rows,), jnp.int32).at[dest].set(sorted_token)
    starts = jnp.arange(n_blocks, dtype=jnp.int32) * row_block
    block_expert = jnp.minimum(lax.optimization_barrier(jnp.sum((pad_end[None, :] <= starts[:, None]).astype(jnp.int32), axis=1)), EXPERTS - 1).astype(jnp.int32)
    quarter = FF // N_TP

    def run_block(inputs):
        rows, index = inputs
        picked = normed[rows]
        gated = jnp.dot(picked, expert_gate[index], preferred_element_type=jnp.float32)
        upward = jnp.dot(picked, expert_up[index], preferred_element_type=jnp.float32)
        hidden = (jax.nn.silu(gated) * upward).astype(jnp.bfloat16)
        pieces = hidden.reshape(row_block, N_TP, quarter).astype(jnp.float32)
        downs = expert_down[index].reshape(N_TP, quarter, D).astype(jnp.float32)
        partial_value = jnp.einsum('rqf,qfd->qrd', pieces, downs).astype(jnp.bfloat16)
        return lax.optimization_barrier(jnp.sum(partial_value.astype(jnp.float32), axis=0)).astype(jnp.bfloat16)
    outputs = lax.map(run_block, (row_token.reshape(n_blocks, row_block), block_expert)).reshape(n_rows, D)
    slot = jnp.zeros((routes,), jnp.int32).at[order].set(dest)
    return outputs[slot]

def reference(stream, conv_value, conv_gate, doc_ids, conv_taps, conv_bias, chan_gain, chan_shift, out_weight, rms_gain, expert_ids, group_prob, route_logits, expert_gate, expert_up, expert_down):
    reach = WIDTH - 1
    values = jnp.concatenate([jnp.zeros((reach, CONV_CH), jnp.bfloat16), conv_value], axis=0)
    gates = jnp.concatenate([jnp.zeros((reach, CONV_CH), jnp.bfloat16), conv_gate], axis=0)
    docs = jnp.concatenate([jnp.full((reach,), -1, jnp.int32), doc_ids.astype(jnp.int32)], axis=0)
    conved = causal_conv(values, gates, docs, conv_taps, conv_bias)
    activated = channel_norm(conved, chan_gain, chan_shift)
    projected = jnp.dot(activated, out_weight, preferred_element_type=jnp.float32)
    resid = (stream.astype(jnp.float32) + projected).astype(jnp.bfloat16)
    normed = rms_norm(resid, rms_gain)
    weights = route_weights(group_prob, route_logits)
    routed = run_experts(normed, expert_ids, expert_gate, expert_up, expert_down)
    combined = lax.optimization_barrier(jnp.sum(weights[:, :, None] * routed.reshape(TOKENS, TOPK, D).astype(jnp.float32), axis=1))
    return (resid.astype(jnp.float32) + combined).astype(jnp.bfloat16)
```

```python
import jax
import jax.numpy as jnp
from jax import lax
from jax.sharding import Mesh, PartitionSpec as P

eps = 1e-06
F32, BF16 = jnp.float32, jnp.bfloat16


def swap(x, axis, by):
    size = lax.axis_size(axis)
    return lax.ppermute(x, axis, [(i, (i + by) % size) for i in range(size)])


def gather_pieces(weight):
    nx, nc = lax.axis_size("tx"), lax.axis_size("tc")
    me = lax.axis_index("tx")
    pieces = []
    for by in range(nx):
        piece = lax.dynamic_index_in_dim(weight, lax.rem(me + by, nx), 0, keepdims=False)
        pieces.append(piece if by == 0 else swap(piece, "tx", by))
    return pieces + [swap(p, "tc", by) for by in range(1, nc) for p in pieces]


def body(
    stream, conv_value, conv_gate, doc_ids, conv_taps, conv_bias, chan_gain, chan_shift, out_weight,
    rms_gain, expert_ids, group_prob, route_logits, expert_gate, expert_up, expert_down,
):
    reach = conv_taps.shape[0] - 1
    tp = ("tx", "tc")
    own_rows, width = stream.shape
    sp_count = lax.axis_size("sp")
    block, chans = conv_value.shape
    docs_row = doc_ids.astype(BF16)
    tail = jnp.concatenate(
        [conv_value[-reach:], conv_gate[-reach:], jnp.broadcast_to(docs_row[-reach:, None], (reach, chans))], axis=0
    )
    tail = lax.ppermute(tail, "sp", [(i, i + 1) for i in range(sp_count - 1)])
    gates_w, ups_w, downs_w = gather_pieces(expert_gate), gather_pieces(expert_up), gather_pieces(expert_down)

    values = jnp.concatenate([tail[:reach], conv_value], axis=0).astype(F32)
    gates = jnp.concatenate([tail[reach : 2 * reach], conv_gate], axis=0).astype(F32)
    docs = jnp.concatenate([tail[2 * reach :, 0], docs_row], axis=0)
    acts = values * jax.nn.sigmoid(gates)
    result = jnp.broadcast_to(conv_bias[None, :], (block, chans))
    for offset in range(reach + 1):
        begin = reach - offset
        same = (docs[begin : begin + block] == docs_row)[:, None]
        result = result + jnp.where(same, acts[begin : begin + block], 0.0) * conv_taps[offset][None, :]
    conved = lax.all_to_all(result.astype(BF16), tp, split_axis=0, concat_axis=1, tiled=True)

    floats = conved.astype(F32)
    mean = jnp.mean(floats, axis=1, keepdims=True)
    spread = jnp.mean(floats * floats, axis=1, keepdims=True) - mean * mean
    activated = jax.nn.silu((floats - mean) * lax.rsqrt(spread + eps) * chan_gain + chan_shift).astype(BF16)
    projected = jnp.dot(activated, out_weight, preferred_element_type=F32)
    resid = (stream.astype(F32) + projected).astype(BF16)
    resid_float = resid.astype(F32)
    mean_square = jnp.mean(resid_float * resid_float, axis=-1, keepdims=True)
    normed = (resid_float * lax.rsqrt(mean_square + eps) * rms_gain).astype(BF16)

    local_experts = expert_gate.shape[0]
    experts_all = sp_count * local_experts
    top_count = expert_ids.shape[1]
    capacity = max(2, 3 * own_rows * top_count // (2 * experts_all))
    gap = route_logits[:, 0] - route_logits[:, 1]
    weights = [group_prob * jax.nn.sigmoid(gap), group_prob * jax.nn.sigmoid(-gap)]
    names = [
        (jnp.arange(experts_all, dtype=jnp.int32)[:, None] == expert_ids[:, k][None, :]).astype(F32)
        for k in range(top_count)
    ]
    named = sum(names)
    weighted = sum(n * w[None, :] for n, w in zip(names, weights))
    order = jnp.arange(own_rows, dtype=jnp.int32)
    before = (order[:, None] < order[None, :]).astype(BF16)
    ranks = jnp.dot(named.astype(BF16), before, preferred_element_type=F32)
    slots = jnp.arange(capacity, dtype=jnp.int32).astype(F32)
    picks = (ranks[:, None, :] == slots[None, :, None]) & (named[:, None, :] > 0)
    picks = picks.reshape(experts_all * capacity, own_rows)
    outgoing = jnp.dot(picks.astype(BF16), normed, preferred_element_type=F32).astype(BF16)
    outgoing = outgoing.reshape(experts_all, capacity, width)
    arrived = lax.all_to_all(outgoing, ("sp", "tx"), split_axis=0, concat_axis=0, tiled=True)
    rows = arrived.reshape(-1, width)
    total = None
    for gate, up, down in zip(gates_w, ups_w, downs_w):
        gated = jnp.dot(rows, gate, preferred_element_type=F32)
        upward = jnp.dot(rows, up, preferred_element_type=F32)
        hidden = (jax.nn.silu(gated) * upward).astype(BF16)
        part = jnp.dot(hidden, down, preferred_element_type=F32)
        total = part if total is None else total + part
    routed = lax.all_to_all(
        total.astype(BF16).reshape(arrived.shape), ("sp", "tx"), split_axis=0, concat_axis=0, tiled=True
    ).reshape(-1, width)
    spots = jnp.where(picks, jnp.repeat(weighted, capacity, axis=0), 0.0)
    high = spots.astype(BF16)
    low = (spots - high.astype(F32)).astype(BF16)
    both = jnp.concatenate([high, low], axis=1)
    mixed = lax.dot_general(both, routed, (((0,), (0,)), ((), ())), preferred_element_type=F32)
    return (resid_float + mixed[:own_rows] + mixed[own_rows:]).astype(BF16)


def solution(mesh):
    sp, tp = mesh.shape["sp"], mesh.shape["tp"]

    def whole(*args):
        nx = args[13].shape[0] // sp
        fine = Mesh(mesh.devices.reshape(sp, nx, tp // nx), ("sp", "tx", "tc"))
        t = ("tx", "tc")
        placed = (
            P(("sp",) + t, None), P("sp", t), P("sp", t), P("sp"), P(None, t), P(t), P(), P(), P(), P(),
            P(("sp",) + t, None), P(("sp",) + t), P(("sp",) + t, None),
            P("sp", None, t), P("sp", None, t), P("sp", t, None),
        )
        return jax.shard_map(
            body, mesh=fine, in_specs=placed, out_specs=P(("sp",) + t, None), check_vma=False
        )(*args)

    return whole
```

```python
import functools

import jax
import jax.numpy as jnp
from jax import lax
from jax.experimental import pallas as pl
from jax.experimental.pallas import tpu as pltpu
from jax.sharding import PartitionSpec as P

eps = 1e-06
F32, BF16 = jnp.float32, jnp.bfloat16
MESH = pl.DeviceIdType.MESH


def flipped(index, mask):
    bit = 1
    while bit <= mask:
        if mask & bit:
            index = index + bit * (1 - 2 * lax.rem(lax.div(index, bit), 2))
        bit *= 2
    return index


def exchange_kernel(
    sp, local, slab_rows, groups,
    out_ref, gate_ref, up_ref, down_ref, ret_ref,
    rows, x_buf, hid_buf, own, part_send, part_recv, back, wg, wu, wd,
    disp_sems, relay_sems, part_sems, back_sems, weight_sems, fetch_sems,
):
    s, t = lax.axis_index("sp"), lax.axis_index("tp")
    h, l = lax.div(t, local), lax.rem(t, local)
    half = slab_rows // 2
    across = (s, (1 - h) * local + l)
    count = sp * local
    own_expert = s * local + l

    def peer(slot):
        m, dl = divmod(slot, local)
        return flipped(s, m), flipped(l, dl)

    def device(slot):
        ps, plocal = peer(slot)
        return (ps, h * local + plocal)

    def remote(src, dst, sems, slot, where):
        return pltpu.make_async_remote_copy(
            src_ref=src, dst_ref=dst, send_sem=sems.at[0, slot], recv_sem=sems.at[1, slot],
            device_id=where, device_id_type=MESH,
        )

    barrier = pltpu.get_barrier_semaphore()
    for slot in range(1, count):
        pl.semaphore_signal(barrier, inc=1, device_id=device(slot), device_id_type=MESH)
    pl.semaphore_signal(barrier, inc=1, device_id=across, device_id_type=MESH)
    pl.semaphore_wait(barrier, count)

    relay, part, back_copies = {}, {}, {}
    dispatch = {}
    for first, last in groups[1:] + groups[:1]:
        for slot in range(first, last):
            if slot:
                ps, plocal = peer(slot)
                dispatch[slot] = remote(
                    out_ref.at[ps * local + plocal], rows.at[0, slot], disp_sems, slot, device(slot)
                )
                dispatch[slot].start()
    relay[0] = remote(out_ref.at[own_expert], rows.at[1, 0], relay_sems, 0, across)
    relay[0].start()
    weights, fetches = [], []
    for k, (src, dst) in enumerate(((gate_ref, wg), (up_ref, wu), (down_ref, wd))):
        fetch = pltpu.make_async_copy(src.at[l], dst.at[0], fetch_sems.at[k])
        fetch.start()
        fetches.append(fetch)
        for dl in range(1, local):
            copy = remote(
                src.at[flipped(l, dl)], dst.at[dl], weight_sems, k * local + dl, (s, h * local + flipped(l, dl))
            )
            copy.start()
            weights.append(copy)
    rows[0, 0] = out_ref[own_expert]

    def pass_across(g):
        for slot in range(*groups[g]):
            if slot:
                dispatch[slot].wait_recv()
                relay[slot] = remote(rows.at[0, slot], rows.at[1, slot], relay_sems, slot, across)
                relay[slot].start()

    size = (groups[0][1] - groups[0][0]) * half
    deep = out_ref.shape[2]

    def compute(g):
        first, last = groups[g]
        for slot in range(first, last):
            relay[slot].wait_recv()
        for plane in range(2):
            slabs = rows[plane, first:last].astype(F32)
            for side in range(2):
                x_buf[plane * size : (plane + 1) * size, side * deep : (side + 1) * deep] = (
                    slabs[:, side * half : (side + 1) * half].reshape(size, deep).astype(BF16)
                )
        for dl in range(local):
            x = x_buf[...]
            gated = jnp.dot(x, wg[dl], preferred_element_type=F32)
            upward = jnp.dot(x, wu[dl], preferred_element_type=F32)
            hid_buf[dl] = (jax.nn.silu(gated) * upward).astype(BF16)
        step = min(256, deep)

        for at in range(0, deep, step):
            sides = []
            for side in range(2):
                total = None
                for dl in range(local):
                    term = jnp.dot(
                        hid_buf[dl], wd[dl, :, side * deep + at : side * deep + at + step],
                        preferred_element_type=F32,
                    )
                    total = term if total is None else total + term
                sides.append(total.reshape(2, last - first, half, step))
            slabs = jnp.concatenate(sides, axis=2)
            own[first:last, :, at : at + step] = slabs[0]
            part_send[first:last, :, at : at + step] = slabs[1].astype(BF16)
        for slot in range(first, last):
            part[slot] = remote(part_send.at[slot], part_recv.at[slot], part_sems, slot, across)
            part[slot].start()

    def finish(g):
        for slot in range(*groups[g]):
            part[slot].wait_recv()
            total = (own[slot] + part_recv[slot].astype(F32)).astype(BF16)
            if slot == 0:
                ret_ref[own_expert] = total
            else:
                back[slot] = total
                back_copies[slot] = remote(back.at[slot], ret_ref.at[own_expert], back_sems, slot, device(slot))
                back_copies[slot].start()

    pass_across(0)
    for copy in fetches:
        copy.wait()
    for copy in weights:
        copy.wait_recv()
    amount = len(groups)
    for g in range(amount + 2):
        if 1 <= g < amount:
            pass_across(g)
        if 1 <= g <= amount:
            compute(g - 1)
        if g >= 2:
            finish(g - 2)
    for slot in range(1, count):
        back_copies[slot].wait_recv()
    for copies in (dispatch, relay, part, back_copies):
        for copy in copies.values():
            copy.wait_send()
    for copy in weights:
        copy.wait_send()


def run_experts(outgoing, expert_gate, expert_up, expert_down):
    sp = lax.axis_size("sp")
    count, slab_rows, deep = outgoing.shape
    local = expert_gate.shape[0]
    quarter = count // 4
    groups = [(0, quarter), (2 * quarter, 3 * quarter), (quarter, 2 * quarter), (3 * quarter, count)]
    slabs = (count, slab_rows, deep)
    m = quarter * slab_rows
    sems = pltpu.SemaphoreType.DMA((2, count))
    return pl.pallas_call(
        functools.partial(exchange_kernel, sp, local, slab_rows, groups),
        out_shape=jax.ShapeDtypeStruct(slabs, BF16),
        in_specs=[pl.BlockSpec(memory_space=pltpu.VMEM)] + [pl.BlockSpec(memory_space=pl.ANY)] * 3,
        out_specs=pl.BlockSpec(memory_space=pltpu.VMEM),
        scratch_shapes=[
            pltpu.VMEM((2,) + slabs, BF16),
            pltpu.VMEM((m, 2 * deep), BF16),
            pltpu.VMEM((local, m, expert_gate.shape[2]), BF16),
            pltpu.VMEM(slabs, F32),
            pltpu.VMEM(slabs, BF16),
            pltpu.VMEM(slabs, BF16),
            pltpu.VMEM(slabs, BF16),
            pltpu.VMEM(expert_gate.shape, BF16),
            pltpu.VMEM(expert_up.shape, BF16),
            pltpu.VMEM(expert_down.shape, BF16),
            sems, sems, sems, sems,
            pltpu.SemaphoreType.DMA((2, 3 * local)),
            pltpu.SemaphoreType.DMA((3,)),
        ],
        compiler_params=pltpu.CompilerParams(
            collective_id=0, has_side_effects=True, vmem_limit_bytes=60 * 1024 * 1024
        ),
    )(outgoing, expert_gate, expert_up, expert_down)


def body(
    stream, conv_value, conv_gate, doc_ids, conv_taps, conv_bias, chan_gain, chan_shift, out_weight,
    rms_gain, expert_ids, group_prob, route_logits, expert_gate, expert_up, expert_down,
):
    reach = conv_taps.shape[0] - 1
    tp = "tp"
    own_rows, width = stream.shape
    sp_count = lax.axis_size("sp")
    block, chans = conv_value.shape
    docs_row = doc_ids.astype(BF16)
    tail = jnp.concatenate(
        [conv_value[-reach:], conv_gate[-reach:], jnp.broadcast_to(docs_row[-reach:, None], (reach, chans))], axis=0
    )
    tail = lax.ppermute(tail, "sp", [(i, i + 1) for i in range(sp_count - 1)])

    values = jnp.concatenate([tail[:reach], conv_value], axis=0).astype(F32)
    gates = jnp.concatenate([tail[reach : 2 * reach], conv_gate], axis=0).astype(F32)
    docs = jnp.concatenate([tail[2 * reach :, 0], docs_row], axis=0)
    acts = values * jax.nn.sigmoid(gates)
    result = jnp.broadcast_to(conv_bias[None, :], (block, chans))
    for offset in range(reach + 1):
        begin = reach - offset
        same = (docs[begin : begin + block] == docs_row)[:, None]
        result = result + jnp.where(same, acts[begin : begin + block], 0.0) * conv_taps[offset][None, :]
    conved = lax.all_to_all(result.astype(BF16), tp, split_axis=0, concat_axis=1, tiled=True)

    floats = conved.astype(F32)
    mean = jnp.mean(floats, axis=1, keepdims=True)
    spread = jnp.mean(floats * floats, axis=1, keepdims=True) - mean * mean
    activated = jax.nn.silu((floats - mean) * lax.rsqrt(spread + eps) * chan_gain + chan_shift).astype(BF16)
    projected = jnp.dot(activated, out_weight, preferred_element_type=F32)
    resid = (stream.astype(F32) + projected).astype(BF16)
    resid_float = resid.astype(F32)
    mean_square = jnp.mean(resid_float * resid_float, axis=-1, keepdims=True)
    normed = (resid_float * lax.rsqrt(mean_square + eps) * rms_gain).astype(BF16)

    local_experts = expert_gate.shape[0]
    experts_all = sp_count * local_experts
    top_count = expert_ids.shape[1]
    capacity = max(2, 3 * own_rows * top_count // (2 * experts_all))
    capacity = (capacity + 7) // 8 * 8
    gap = route_logits[:, 0] - route_logits[:, 1]
    weights = [group_prob * jax.nn.sigmoid(gap), group_prob * jax.nn.sigmoid(-gap)]
    names = [
        (jnp.arange(experts_all, dtype=jnp.int32)[:, None] == expert_ids[:, k][None, :]).astype(F32)
        for k in range(top_count)
    ]
    named = sum(names)
    weighted = sum(n * w[None, :] for n, w in zip(names, weights))
    order = jnp.arange(own_rows, dtype=jnp.int32)
    before = (order[:, None] < order[None, :]).astype(BF16)
    ranks = jnp.dot(named.astype(BF16), before, preferred_element_type=F32)
    slots = jnp.arange(capacity, dtype=jnp.int32).astype(F32)
    picks = (ranks[:, None, :] == slots[None, :, None]) & (named[:, None, :] > 0)
    side = jnp.eye(2, dtype=jnp.bool_)[None, :, None, :, None]
    picks = (picks[:, None, :, None, :] & side).reshape(experts_all * 2 * capacity, 2 * own_rows)
    halves = jnp.concatenate([normed[:, : width // 2], normed[:, width // 2 :]], axis=0)
    outgoing = jnp.dot(picks.astype(BF16), halves, preferred_element_type=F32).astype(BF16)
    outgoing = outgoing.reshape(experts_all, 2 * capacity, width // 2)
    routed = run_experts(outgoing, expert_gate, expert_up, expert_down).reshape(-1, width // 2)
    spread_weights = jnp.tile(jnp.repeat(weighted, 2 * capacity, axis=0), (1, 2))
    spots = jnp.where(picks, spread_weights, 0.0)
    high = spots.astype(BF16)
    low = (spots - high.astype(F32)).astype(BF16)
    both = jnp.concatenate([high, low], axis=1)
    mixed = lax.dot_general(both, routed, (((0,), (0,)), ((), ())), preferred_element_type=F32)
    mixed = mixed[: 2 * own_rows] + mixed[2 * own_rows :]
    mixed = jnp.concatenate([mixed[:own_rows], mixed[own_rows:]], axis=1)
    return (resid_float + mixed).astype(BF16)


def solution(mesh):
    placed = (
        P(("sp", "tp"), None), P("sp", "tp"), P("sp", "tp"), P("sp"), P(None, "tp"), P("tp"),
        P(), P(), P(), P(), P(("sp", "tp"), None), P(("sp", "tp")), P(("sp", "tp"), None),
        P("sp", None, "tp"), P("sp", None, "tp"), P("sp", "tp", None),
    )
    return jax.shard_map(
        body, mesh=mesh, in_specs=placed, out_specs=P(("sp", "tp"), None), check_vma=False
    )
```

```python
import functools

import jax
import jax.numpy as jnp
from jax import lax
from jax.experimental import pallas as pl
from jax.experimental.pallas import tpu as pltpu
from jax.sharding import PartitionSpec as P

eps = 1e-06
F32, BF16 = jnp.float32, jnp.bfloat16
MESH = pl.DeviceIdType.MESH


def flipped(index, mask):
    bit = 1
    while bit <= mask:
        if mask & bit:
            index = index + bit * (1 - 2 * lax.rem(lax.div(index, bit), 2))
        bit *= 2
    return index


def exchange_kernel(
    sp, local, slab_rows, groups,
    out_ref, gate_ref, up_ref, down_ref, ret_ref,
    rows, x_buf, hid_buf, own, part_send, part_recv, back, wg, wu, wd,
    disp_sems, relay_sems, part_sems, back_sems, weight_sems, fetch_sems,
):
    s, t = lax.axis_index("sp"), lax.axis_index("tp")
    h, l = lax.div(t, local), lax.rem(t, local)
    half = slab_rows // 2
    across = (s, (1 - h) * local + l)
    count = sp * local
    own_expert = s * local + l

    def peer(slot):
        m, dl = divmod(slot, local)
        return flipped(s, m), flipped(l, dl)

    def device(slot):
        ps, plocal = peer(slot)
        return (ps, h * local + plocal)

    def remote(src, dst, sems, slot, where):
        return pltpu.make_async_remote_copy(
            src_ref=src, dst_ref=dst, send_sem=sems.at[0, slot], recv_sem=sems.at[1, slot],
            device_id=where, device_id_type=MESH,
        )

    barrier = pltpu.get_barrier_semaphore()
    for slot in range(1, count):
        pl.semaphore_signal(barrier, inc=1, device_id=device(slot), device_id_type=MESH)
    pl.semaphore_signal(barrier, inc=1, device_id=across, device_id_type=MESH)
    pl.semaphore_wait(barrier, count)

    relay, part, back_copies = {}, {}, {}
    dispatch = {}
    for first, last in groups[1:] + groups[:1]:
        for slot in range(first, last):
            if slot:
                ps, plocal = peer(slot)
                dispatch[slot] = remote(
                    out_ref.at[ps * local + plocal], rows.at[0, slot], disp_sems, slot, device(slot)
                )
                dispatch[slot].start()
    relay[0] = remote(out_ref.at[own_expert], rows.at[1, 0], relay_sems, 0, across)
    relay[0].start()
    weights, fetches = [], []
    for k, (src, dst) in enumerate(((gate_ref, wg), (up_ref, wu), (down_ref, wd))):
        fetch = pltpu.make_async_copy(src.at[l], dst.at[0], fetch_sems.at[k])
        fetch.start()
        fetches.append(fetch)
        for dl in range(1, local):
            copy = remote(
                src.at[flipped(l, dl)], dst.at[dl], weight_sems, k * local + dl, (s, h * local + flipped(l, dl))
            )
            copy.start()
            weights.append(copy)
    rows[0, 0] = out_ref[own_expert]

    def pass_across(g):
        for slot in range(*groups[g]):
            if slot:
                dispatch[slot].wait_recv()
                relay[slot] = remote(rows.at[0, slot], rows.at[1, slot], relay_sems, slot, across)
                relay[slot].start()

    size = (groups[0][1] - groups[0][0]) * half
    deep = out_ref.shape[2]

    def compute(g):
        first, last = groups[g]
        for slot in range(first, last):
            relay[slot].wait_recv()
        for plane in range(2):
            slabs = rows[plane, first:last].astype(F32)
            for side in range(2):
                x_buf[plane * size : (plane + 1) * size, side * deep : (side + 1) * deep] = (
                    slabs[:, side * half : (side + 1) * half].reshape(size, deep).astype(BF16)
                )
        for dl in range(local):
            x = x_buf[...]
            gated = jnp.dot(x, wg[dl], preferred_element_type=F32)
            upward = jnp.dot(x, wu[dl], preferred_element_type=F32)
            hid_buf[dl] = (jax.nn.silu(gated) * upward).astype(BF16)
        step = min(256, deep)

        for at in range(0, deep, step):
            sides = []
            for side in range(2):
                total = None
                for dl in range(local):
                    term = jnp.dot(
                        hid_buf[dl], wd[dl, :, side * deep + at : side * deep + at + step],
                        preferred_element_type=F32,
                    )
                    total = term if total is None else total + term
                sides.append(total.reshape(2, last - first, half, step))
            slabs = jnp.concatenate(sides, axis=2)
            own[first:last, :, at : at + step] = slabs[0]
            part_send[first:last, :, at : at + step] = slabs[1].astype(BF16)
        for slot in range(first, last):
            part[slot] = remote(part_send.at[slot], part_recv.at[slot], part_sems, slot, across)
            part[slot].start()

    def finish(g):
        for slot in range(*groups[g]):
            part[slot].wait_recv()
            total = (own[slot] + part_recv[slot].astype(F32)).astype(BF16)
            if slot == 0:
                ret_ref[own_expert] = total
            else:
                back[slot] = total
                back_copies[slot] = remote(back.at[slot], ret_ref.at[own_expert], back_sems, slot, device(slot))
                back_copies[slot].start()

    pass_across(0)
    for copy in fetches:
        copy.wait()
    for copy in weights:
        copy.wait_recv()
    amount = len(groups)
    for g in range(amount + 2):
        if 1 <= g < amount:
            pass_across(g)
        if 1 <= g <= amount:
            compute(g - 1)
        if g >= 2:
            finish(g - 2)
    for slot in range(1, count):
        back_copies[slot].wait_recv()
    for copies in (dispatch, relay, part, back_copies):
        for copy in copies.values():
            copy.wait_send()
    for copy in weights:
        copy.wait_send()


def run_experts(outgoing, expert_gate, expert_up, expert_down):
    sp = lax.axis_size("sp")
    count, slab_rows, deep = outgoing.shape
    local = expert_gate.shape[0]
    quarter = count // 4
    groups = [(0, quarter), (2 * quarter, 3 * quarter), (quarter, 2 * quarter), (3 * quarter, count)]
    slabs = (count, slab_rows, deep)
    m = quarter * slab_rows
    sems = pltpu.SemaphoreType.DMA((2, count))
    return pl.pallas_call(
        functools.partial(exchange_kernel, sp, local, slab_rows, groups),
        out_shape=jax.ShapeDtypeStruct(slabs, BF16),
        in_specs=[pl.BlockSpec(memory_space=pltpu.VMEM)] + [pl.BlockSpec(memory_space=pl.ANY)] * 3,
        out_specs=pl.BlockSpec(memory_space=pltpu.VMEM),
        scratch_shapes=[
            pltpu.VMEM((2,) + slabs, BF16),
            pltpu.VMEM((m, 2 * deep), BF16),
            pltpu.VMEM((local, m, expert_gate.shape[2]), BF16),
            pltpu.VMEM(slabs, F32),
            pltpu.VMEM(slabs, BF16),
            pltpu.VMEM(slabs, BF16),
            pltpu.VMEM(slabs, BF16),
            pltpu.VMEM(expert_gate.shape, BF16),
            pltpu.VMEM(expert_up.shape, BF16),
            pltpu.VMEM(expert_down.shape, BF16),
            sems, sems, sems, sems,
            pltpu.SemaphoreType.DMA((2, 3 * local)),
            pltpu.SemaphoreType.DMA((3,)),
        ],
        compiler_params=pltpu.CompilerParams(
            collective_id=0, has_side_effects=True, vmem_limit_bytes=60 * 1024 * 1024
        ),
    )(outgoing, expert_gate, expert_up, expert_down)


def front_kernel(
    sp, tp, capacity, halo,
    value_ref, gate_ref, docs_ref, taps_ref, bias_ref, ids_ref, prob_ref, logits_ref,
    cv_ref, picks_ref, spots_ref,
    tails, acts, docs, conved, halo_sems, cv_sems,
):
    s, t = lax.axis_index("sp"), lax.axis_index("tp")
    following, previous = (lax.rem(s + 1, sp), t), (lax.rem(s + sp - 1, sp), t)
    barrier = pltpu.get_barrier_semaphore()
    peers = [(s, flipped(t, d)) for d in range(1, tp)]
    for where in [following, previous] + peers:
        pl.semaphore_signal(barrier, inc=1, device_id=where, device_id_type=MESH)
    block, chans = value_ref.shape
    own_rows = block // tp
    taps = taps_ref.shape[0]
    value, gate = value_ref[...].astype(F32), gate_ref[...].astype(F32)
    acts[halo:] = value * jax.nn.sigmoid(gate)
    docs[halo:] = docs_ref[...].astype(F32)
    pl.semaphore_wait(barrier, 2 + len(peers))
    tail_copies = []
    for k, ref in enumerate((value_ref, gate_ref, docs_ref)):
        copy = pltpu.make_async_remote_copy(
            src_ref=ref.at[pl.ds(block - halo, halo)], dst_ref=tails.at[k],
            send_sem=halo_sems.at[0, k], recv_sem=halo_sems.at[1, k], device_id=following, device_id_type=MESH,
        )
        copy.start()
        tail_copies.append(copy)

    def convolve(q):
        at = halo + q * own_rows
        own_doc = docs[at : at + own_rows]
        result = jnp.broadcast_to(bias_ref[...], (own_rows, chans))
        for j in range(taps):
            same = docs[at - j : at - j + own_rows] == own_doc
            result = result + jnp.where(same, acts[at - j : at - j + own_rows], 0.0) * taps_ref[j : j + 1]
        conved[q] = result.astype(BF16)

    for q in range(1, tp):
        convolve(q)
    for copy in tail_copies:
        copy.wait_recv()
    tail_value, tail_gate = tails[0].astype(F32), tails[1].astype(F32)
    acts[:halo] = tail_value * jax.nn.sigmoid(tail_gate)
    docs[:halo] = jnp.where(s > 0, tails[2].astype(F32), -1.0)
    convolve(0)
    copies = []
    for d in range(1, tp):
        copy = pltpu.make_async_remote_copy(
            src_ref=conved.at[flipped(t, d)], dst_ref=cv_ref.at[t],
            send_sem=cv_sems.at[0, d], recv_sem=cv_sems.at[1, d],
            device_id=(s, flipped(t, d)), device_id_type=MESH,
        )
        copy.start()
        copies.append(copy)
    cv_ref[t] = conved[t]

    rows = 2 * capacity
    experts = picks_ref.shape[0] // rows
    top_count, tokens = ids_ref.shape
    number = lax.broadcasted_iota(jnp.int32, (experts, tokens), 0)
    gap = logits_ref[0:1] - logits_ref[1:2]
    weights = [prob_ref[...] * jax.nn.sigmoid(gap), prob_ref[...] * jax.nn.sigmoid(-gap)]
    named, weighted = 0.0, 0.0
    for k in range(top_count):
        name = jnp.where(number == ids_ref[k : k + 1], 1.0, 0.0)
        named, weighted = named + name, weighted + name * weights[k]
    earlier = lax.broadcasted_iota(jnp.int32, (tokens, tokens), 0)
    later = lax.broadcasted_iota(jnp.int32, (tokens, tokens), 1)
    before = jnp.where(earlier < later, 1.0, 0.0).astype(BF16)
    ranks = jnp.dot(named.astype(BF16), before, preferred_element_type=F32)
    ranks = jnp.where(named > 0.5, ranks, -1.0)
    place = lax.broadcasted_iota(jnp.int32, (capacity, tokens), 0).astype(F32)
    zeros = jnp.zeros((capacity, tokens), F32)

    def both_halves(x):
        return jnp.concatenate(
            [jnp.concatenate([x, zeros], axis=1), jnp.concatenate([zeros, x], axis=1)], axis=0
        ).astype(BF16)

    for e in range(experts):
        pick = jnp.where(place == ranks[e : e + 1], 1.0, 0.0)
        spot = pick * weighted[e : e + 1]
        high = spot.astype(BF16).astype(F32)
        picks_ref[e * rows : (e + 1) * rows] = both_halves(pick)
        spots_ref[e * rows : (e + 1) * rows, : 2 * tokens] = both_halves(high)
        spots_ref[e * rows : (e + 1) * rows, 2 * tokens :] = both_halves(spot - high)
    for copy in copies:
        copy.wait()
    for copy in tail_copies:
        copy.wait_send()


def front(conv_value, conv_gate, doc_ids, conv_taps, conv_bias, expert_ids, group_prob, route_logits, capacity, experts):
    sp, tp = lax.axis_size("sp"), lax.axis_size("tp")
    block, chans = conv_value.shape
    halo = (conv_taps.shape[0] - 1 + 15) // 16 * 16
    tokens = expert_ids.shape[0]
    rows = experts * 2 * capacity
    docs = jnp.broadcast_to(doc_ids.astype(BF16)[:, None], (block, chans))
    pieces = (tp, block // tp, chans)
    vmem = pl.BlockSpec(memory_space=pltpu.VMEM)
    return pl.pallas_call(
        functools.partial(front_kernel, sp, tp, capacity, halo),
        out_shape=(
            jax.ShapeDtypeStruct(pieces, BF16),
            jax.ShapeDtypeStruct((rows, 2 * tokens), BF16),
            jax.ShapeDtypeStruct((rows, 4 * tokens), BF16),
        ),
        in_specs=[vmem] * 8,
        out_specs=(vmem,) * 3,
        scratch_shapes=[
            pltpu.VMEM((3, halo, chans), BF16),
            pltpu.VMEM((halo + block, chans), F32),
            pltpu.VMEM((halo + block, chans), F32),
            pltpu.VMEM(pieces, BF16),
            pltpu.SemaphoreType.DMA((2, 3)),
            pltpu.SemaphoreType.DMA((2, tp)),
        ],
        compiler_params=pltpu.CompilerParams(collective_id=1, has_side_effects=True),
    )(
        conv_value, conv_gate, docs, conv_taps, conv_bias[None, :],
        expert_ids.T, group_prob[None, :], route_logits.T,
    )


def body(
    stream, conv_value, conv_gate, doc_ids, conv_taps, conv_bias, chan_gain, chan_shift, out_weight,
    rms_gain, expert_ids, group_prob, route_logits, expert_gate, expert_up, expert_down,
):
    own_rows, width = stream.shape
    experts_all = lax.axis_size("sp") * expert_gate.shape[0]
    top_count = expert_ids.shape[1]
    capacity = max(2, 3 * own_rows * top_count // (2 * experts_all))
    capacity = (capacity + 7) // 8 * 8
    conved, picks, spots = front(
        conv_value, conv_gate, doc_ids, conv_taps, conv_bias, expert_ids, group_prob, route_logits,
        capacity, experts_all,
    )
    conved = jnp.swapaxes(conved, 0, 1).reshape(own_rows, -1)
    floats = conved.astype(F32)
    mean = jnp.mean(floats, axis=1, keepdims=True)
    spread = jnp.mean(floats * floats, axis=1, keepdims=True) - mean * mean
    activated = jax.nn.silu((floats - mean) * lax.rsqrt(spread + eps) * chan_gain + chan_shift).astype(BF16)
    projected = jnp.dot(activated, out_weight, preferred_element_type=F32)
    resid = (stream.astype(F32) + projected).astype(BF16)
    resid_float = resid.astype(F32)
    mean_square = jnp.mean(resid_float * resid_float, axis=-1, keepdims=True)
    normed = (resid_float * lax.rsqrt(mean_square + eps) * rms_gain).astype(BF16)

    halves = jnp.concatenate([normed[:, : width // 2], normed[:, width // 2 :]], axis=0)
    outgoing = jnp.dot(picks, halves, preferred_element_type=F32).astype(BF16)
    outgoing = outgoing.reshape(experts_all, 2 * capacity, width // 2)
    routed = run_experts(outgoing, expert_gate, expert_up, expert_down).reshape(-1, width // 2)
    mixed = lax.dot_general(spots, routed, (((0,), (0,)), ((), ())), preferred_element_type=F32)
    mixed = mixed[: 2 * own_rows] + mixed[2 * own_rows :]
    mixed = jnp.concatenate([mixed[:own_rows], mixed[own_rows:]], axis=1)
    return (resid_float + mixed).astype(BF16)


def solution(mesh):
    placed = (
        P(("sp", "tp"), None), P("sp", "tp"), P("sp", "tp"), P("sp"), P(None, "tp"), P("tp"),
        P(), P(), P(), P(), P(("sp", "tp"), None), P(("sp", "tp")), P(("sp", "tp"), None),
        P("sp", None, "tp"), P("sp", None, "tp"), P("sp", "tp", None),
    )
    return jax.shard_map(
        body, mesh=mesh, in_specs=placed, out_specs=P(("sp", "tp"), None), check_vma=False
    )
```
